32 devices in a mesh: sp: 16 (over z, y, x), tp: 2 (over core).
Axes of the slice: x: 2, y: 2, z: 4, core: 2. Of those that a mesh axis runs over, the one named last changes fastest.
Arguments:
- residual: bfloat16 [2048, 2048], P('sp'), may hold values from -6 to 6
- query_nope: bfloat16 [2048, 8, 128], P('sp', 'tp'), may hold values from -6 to 6
- query_rope: bfloat16 [2048, 8, 64], P('sp', 'tp'), may hold values from -64 to 64
- latent: bfloat16 [2048, 256], P('sp'), may hold values from -6 to 6
- rope_key: bfloat16 [2048, 64], P('sp'), may hold values from -64 to 64
- kv_gain: bfloat16 [256], replicated, may hold values from 0.099609375 to 1.8984375
- key_up: bfloat16 [256, 8, 128], replicated, may hold values from -0.375 to 0.375
- value_up: bfloat16 [256, 8, 128], replicated, may hold values from -0.375 to 0.375
- out_weight: bfloat16 [1024, 2048], P('tp'), may hold values from -0.1875 to 0.1875
- post_gain: bfloat16 [2048], replicated, may hold values from 0.099609375 to 1.8984375
- pre_gain: bfloat16 [2048], replicated, may hold values from 0.099609375 to 1.8984375
- ffn_gain: bfloat16 [2048], replicated, may hold values from 0.099609375 to 1.8984375
- up_value: bfloat16 [2048, 5632], P('sp', 'tp'), may hold values from -0.125 to 0.125
- up_gate: bfloat16 [2048, 5632], P('sp', 'tp'), may hold values from -0.125 to 0.125
- conv_value: bfloat16 [3, 5632], replicated, may hold values from -3.5 to 3.5
- conv_gate: bfloat16 [3, 5632], replicated, may hold values from -3.5 to 3.5
- down_weight: bfloat16 [5632, 2048], P('tp', 'sp'), may hold values from -0.078125 to 0.078125
Outputs:
- layer_out: bfloat16 [2048, 2048], P(('sp', 'tp'))
The draws below stay inside these ranges and needn't reach their ends.
All inputs are finite; a program needn't handle non-finite values.
Results may differ from the reference program's by a relative error of at most 0.02.
Values may be sent and summed in bfloat16 or wider, within the bound.
A program may use at most 128 MiB of HBM per device.

```python
import jax
import jax.numpy as jnp
from jax import lax

D = 2048
HEADS = 8
NOPE = 128
ROPE = 64
VD = 128
KV = 256
FF = 5632
GRID = 64
TOKENS = 2048
N_TP = 2


def drawn_pair(key):
    folded = jax.random.fold_in(key, 41)
    query_key, rope_seed = jax.random.split(folded, 2)
    queries = jax.random.normal(query_key, (TOKENS, HEADS, ROPE), jnp.float32)
    rope_keys = jax.random.normal(rope_seed, (TOKENS, ROPE), jnp.float32)
    return (jnp.clip(queries, -64.0, 64.0), jnp.clip(rope_keys, -64.0, 64.0))


def draw_query_rope(key, part):
    return drawn_pair(key)[0].astype(jnp.bfloat16)


def draw_rope_key(key, part):
    return drawn_pair(key)[1].astype(jnp.bfloat16)


def level_of(key, shape, cuts, smallest, top_value):
    loudness = 1.0
    for dim, parts in cuts:
        draws = jax.random.uniform(jax.random.fold_in(jax.random.fold_in(key, 6), dim), (parts,), jnp.float32, smallest / len(cuts), top_value / len(cuts))
        loudness = loudness * jnp.repeat(jnp.exp(draws), shape[dim] // parts).reshape((-1,) + (1,) * (len(shape) - 1 - dim))
    return loudness


def bell_draw(rng, dims, scale, most, cuts=(), held_as=jnp.bfloat16):
    entries = scale * jax.random.normal(rng, dims, jnp.float32)
    if cuts:
        entries = entries * level_of(rng, dims, cuts, -0.22, 0.18)
    return jnp.clip(entries, -most, most).astype(held_as)


def setup_inputs(seed: int = 0) -> dict:
    arg_keys = jax.random.split(jax.random.key(seed), 18)
    return {
        "residual": bell_draw(arg_keys[0], (TOKENS, D), 1.0, 6.0, ((0, 16),)),
        "query_nope": bell_draw(arg_keys[1], (TOKENS, HEADS, NOPE), 1.0, 6.0, ((0, 16), (1, 2))),
        "query_rope": draw_query_rope(jax.random.fold_in(arg_keys[17], 71), 0),
        "latent": bell_draw(arg_keys[3], (TOKENS, KV), 1.0, 6.0, ((0, 16),)),
        "rope_key": draw_rope_key(jax.random.fold_in(arg_keys[17], 71), 0),
        "kv_gain": jnp.clip(1.0 + 0.18 * jax.random.normal(arg_keys[5], (KV,), jnp.float32), 0.099609375, 1.8984375).astype(jnp.bfloat16),
        "key_up": bell_draw(arg_keys[6], (KV, HEADS, NOPE), KV ** -0.5, 0.375),
        "value_up": bell_draw(arg_keys[7], (KV, HEADS, VD), KV ** -0.5, 0.375),
        "out_weight": bell_draw(arg_keys[8], (HEADS * VD, D), (HEADS * VD) ** -0.5, 0.1875, ((0, 2),)),
        "post_gain": jnp.clip(1.0 + 0.18 * jax.random.normal(arg_keys[9], (D,), jnp.float32), 0.099609375, 1.8984375).astype(jnp.bfloat16),
        "pre_gain": jnp.clip(1.0 + 0.18 * jax.random.normal(arg_keys[10], (D,), jnp.float32), 0.099609375, 1.8984375).astype(jnp.bfloat16),
        "ffn_gain": jnp.clip(1.0 + 0.18 * jax.random.normal(arg_keys[11], (D,), jnp.float32), 0.099609375, 1.8984375).astype(jnp.bfloat16),
        "up_value": bell_draw(arg_keys[12], (D, FF), D ** -0.5, 0.125, ((0, 16), (1, 2))),
        "up_gate": bell_draw(arg_keys[13], (D, FF), D ** -0.5, 0.125, ((0, 16), (1, 2))),
        "conv_value": bell_draw(arg_keys[14], (3, FF), 3 ** -0.5, 3.5),
        "conv_gate": bell_draw(arg_keys[15], (3, FF), 3 ** -0.5, 3.5),
        "down_weight": bell_draw(arg_keys[16], (FF, D), FF ** -0.5, 0.078125, ((0, 2), (1, 16))),
    }


epsilon = 1e-06
rope_base = 10000.0

def rms_norm(values, gain):
    return values * lax.rsqrt(lax.optimization_barrier(jnp.mean(values * values, axis=-1, keepdims=True)) + epsilon) * gain.astype(jnp.float32)

def widened(values):
    return lax.optimization_barrier(values.astype(jnp.bfloat16)).astype(jnp.float32)

def rotate(values, positions):
    pair_count = values.shape[-1] // 4
    frequency = rope_base ** (-jnp.arange(pair_count, dtype=jnp.float32) / pair_count)
    grid_rows = (positions // GRID).astype(jnp.float32)
    grid_cols = (positions % GRID).astype(jnp.float32)
    angles = jnp.stack([grid_rows, grid_cols], axis=-1)[:, :, None] * frequency
    table_shape = (angles.shape[0],) + (1,) * (values.ndim - 2) + angles.shape[1:]
    cosine = jnp.cos(angles).reshape(table_shape)
    sine = jnp.sin(angles).reshape(table_shape)
    halves = values.reshape(values.shape[:-1] + (2, 2, pair_count))
    leading = halves[..., 0, :]
    trailing = halves[..., 1, :]
    turned = jnp.stack([leading * cosine - trailing * sine, trailing * cosine + leading * sine], axis=-2)
    return turned.reshape(values.shape)

def reference(residual, query_nope, query_rope, latent, rope_key, kv_gain, key_up, value_up, out_weight, post_gain, pre_gain, ffn_gain, up_value, up_gate, conv_value, conv_gate, down_weight):
    token_count = residual.shape[0]
    positions = jnp.arange(token_count, dtype=jnp.int32)
    score_scale = (NOPE + ROPE) ** (-0.5)
    normed_wide = widened(rms_norm(latent.astype(jnp.float32), kv_gain))
    keys_nope = widened(jnp.einsum('nc,chd->nhd', normed_wide, key_up.astype(jnp.float32)))
    values_all = widened(jnp.einsum('nc,chd->nhd', normed_wide, value_up.astype(jnp.float32)))
    key_turn = widened(rotate(rope_key.astype(jnp.float32), positions))
    query_turn = widened(rotate(query_rope.astype(jnp.float32), positions))
    keys_all = jnp.concatenate([keys_nope, jnp.broadcast_to(key_turn[:, None, :], (token_count, HEADS, ROPE))], axis=-1)
    queries = jnp.concatenate([query_nope.astype(jnp.float32), query_turn], axis=-1)
    block_size = min(512, token_count)
    query_blocks = queries.reshape(token_count // block_size, block_size, HEADS, NOPE + ROPE)

    def attend_block(query_block):
        scores = jnp.einsum('qhd,khd->hqk', query_block, keys_all) * score_scale
        row_max = lax.optimization_barrier(jnp.max(scores, axis=-1, keepdims=True))
        weights = jnp.exp(scores - row_max)
        totals = lax.optimization_barrier(jnp.sum(weights, axis=-1))
        mixed = jnp.einsum('hqk,khd->qhd', widened(weights), values_all)
        return (mixed / jnp.transpose(totals)[:, :, None]).astype(jnp.bfloat16)
    attended = lax.map(attend_block, query_blocks).reshape(token_count, HEADS * VD)
    group_width = HEADS * VD // N_TP

    def add_heads(running, group_id):
        block_rows = lax.dynamic_slice_in_dim(attended, group_id * group_width, group_width, 1)
        weight_rows = lax.dynamic_slice_in_dim(out_weight, group_id * group_width, group_width, 0)
        partial_value = jnp.dot(block_rows, weight_rows, preferred_element_type=jnp.float32)
        return (running + widened(partial_value), None)
    summed = lax.scan(add_heads, jnp.zeros((token_count, D), jnp.float32), jnp.arange(N_TP, dtype=jnp.int32))[0]
    stream_wide = widened(residual.astype(jnp.float32) + rms_norm(widened(summed), post_gain))
    inputs = rms_norm(stream_wide, pre_gain).astype(jnp.bfloat16)
    value_rows = widened(jnp.dot(inputs, up_value, preferred_element_type=jnp.float32))
    gate_rows = widened(jnp.dot(inputs, up_gate, preferred_element_type=jnp.float32))

    def convolve(rows_wide, conv_taps):
        padded = jnp.pad(rows_wide, ((1, 1), (0, 0)))
        return padded[:-2] * conv_taps[0] + padded[1:-1] * conv_taps[1] + padded[2:] * conv_taps[2]
    value_conv = convolve(value_rows, conv_value.astype(jnp.float32))
    gate_conv = convolve(gate_rows, conv_gate.astype(jnp.float32))
    hidden = (jax.nn.silu(gate_conv) * value_conv).astype(jnp.bfloat16)
    ff_width = FF // N_TP

    def add_units(running, group_id):
        block_rows = lax.dynamic_slice_in_dim(hidden, group_id * ff_width, ff_width, 1)
        weight_rows = lax.dynamic_slice_in_dim(down_weight, group_id * ff_width, ff_width, 0)
        partial_value = jnp.dot(block_rows, weight_rows, preferred_element_type=jnp.float32)
        return (running + widened(partial_value), None)
    projected = lax.scan(add_units, jnp.zeros((token_count, D), jnp.float32), jnp.arange(N_TP, dtype=jnp.int32))[0]
    return (stream_wide + rms_norm(widened(projected), ffn_gain)).astype(jnp.bfloat16)
```

```python
import jax
import jax.numpy as jnp
from jax import lax
from jax.sharding import PartitionSpec as P

GRID = 64


epsilon = 1e-06
rope_base = 10000.0


def extended(x, sides, width):
    for axis, dim in sides:
        size, length = (lax.axis_size(axis), x.shape[dim])
        up = [(i, (i + 1) % size) for i in range(size - 1)]
        down = [(j, i) for i, j in up]
        last = lax.slice_in_dim(x, length - width, length, axis=dim)
        initial = lax.slice_in_dim(x, 0, width, axis=dim)
        before = lax.ppermute(last, axis, up)
        after = lax.ppermute(initial, axis, down)
        x = jnp.concatenate([before, x, after], axis=dim)
    return x


def rms_norm(values, gain):
    return (
        values
        * lax.rsqrt(jnp.mean(values * values, axis=-1, keepdims=True) + epsilon)
        * gain.astype(jnp.float32)
    )


def widened(values):
    return lax.optimization_barrier(values.astype(jnp.bfloat16)).astype(jnp.float32)


def rotate(values, positions):
    pair_count = values.shape[-1] // 4
    frequency = rope_base ** (-jnp.arange(pair_count, dtype=jnp.float32) / pair_count)
    grid_rows = (positions // GRID).astype(jnp.float32)
    grid_cols = (positions % GRID).astype(jnp.float32)
    angles = jnp.stack([grid_rows, grid_cols], axis=-1)[:, :, None] * frequency
    table_shape = (angles.shape[0],) + (1,) * (values.ndim - 2) + angles.shape[1:]
    cosine = jnp.cos(angles).reshape(table_shape)
    sine = jnp.sin(angles).reshape(table_shape)
    halves = values.reshape(values.shape[:-1] + (2, 2, pair_count))
    leading = halves[..., 0, :]
    trailing = halves[..., 1, :]
    turned = jnp.stack(
        [leading * cosine - trailing * sine, trailing * cosine + leading * sine], axis=-2
    )
    return turned.reshape(values.shape)


def feed_by_units(
    own_inputs, stream_wide, up_value, up_gate, conv_value, conv_gate, down_weight, ffn_gain
):
    sp_size = lax.axis_size("sp")
    ff_dev = up_value.shape[1]
    unit = ff_dev // sp_size
    first_unit = lax.axis_index("tp") * ff_dev + lax.axis_index("sp") * unit
    up_pair = jnp.stack(
        [up_value.reshape(-1, sp_size, unit), up_gate.reshape(-1, sp_size, unit)], axis=0
    )
    up_mine = lax.all_to_all(up_pair, "sp", split_axis=2, concat_axis=1, tiled=True)[:, :, 0]
    down_mine = lax.all_to_all(down_weight, "sp", split_axis=0, concat_axis=1, tiled=True)
    inputs = lax.all_gather(own_inputs, ("sp", "tp"), axis=0, tiled=True)

    def conved(weight, taps):
        rows = jnp.dot(inputs, weight, preferred_element_type=jnp.float32).astype(jnp.bfloat16)
        padded = jnp.pad(rows, ((1, 1), (0, 0))).astype(jnp.float32)
        taps = lax.dynamic_slice_in_dim(taps, first_unit, unit, 1).astype(jnp.float32)
        return padded[:-2] * taps[0] + padded[1:-1] * taps[1] + padded[2:] * taps[2]

    hidden = jax.nn.silu(conved(up_mine[1], conv_gate)) * conved(up_mine[0], conv_value)
    terms = jnp.dot(
        hidden.astype(jnp.bfloat16), down_mine, preferred_element_type=jnp.float32
    ).astype(jnp.bfloat16)
    reduced = lax.psum_scatter(terms, ("sp", "tp"), scatter_dimension=0, tiled=True)
    reduced = widened(reduced.astype(jnp.float32))
    return (stream_wide + rms_norm(reduced, ffn_gain)).astype(jnp.bfloat16)


def body(
    residual,
    query_nope,
    query_rope,
    latent,
    rope_key,
    kv_gain,
    key_up,
    value_up,
    out_weight,
    post_gain,
    pre_gain,
    ffn_gain,
    up_value,
    up_gate,
    conv_value,
    conv_gate,
    down_weight,
):
    tok_rows = residual.shape[0]
    heads_dev = query_nope.shape[1]
    value_width = value_up.shape[2]
    tp_index = lax.axis_index("tp")
    positions = lax.axis_index("sp") * tok_rows + jnp.arange(tok_rows, dtype=jnp.int32)
    score_scale = (query_nope.shape[2] + query_rope.shape[2]) ** (-0.5)
    normed = rms_norm(latent.astype(jnp.float32), kv_gain).astype(jnp.bfloat16)
    key_turn = rotate(rope_key.astype(jnp.float32), positions).astype(jnp.bfloat16)
    query_turn = rotate(query_rope.astype(jnp.float32), positions).astype(jnp.bfloat16)
    key_local = lax.dynamic_slice_in_dim(key_up, tp_index * heads_dev, heads_dev, 1)
    value_local = lax.dynamic_slice_in_dim(value_up, tp_index * heads_dev, heads_dev, 1)
    pieces = (
        lax.all_gather(normed, "sp", axis=0, tiled=True),
        lax.all_gather(key_turn, "sp", axis=0, tiled=True),
    )
    keys_nope = jnp.einsum(
        "nc,chd->nhd", pieces[0], key_local, preferred_element_type=jnp.float32
    ).astype(jnp.bfloat16)
    values_part = jnp.einsum(
        "nc,chd->nhd", pieces[0], value_local, preferred_element_type=jnp.float32
    ).astype(jnp.bfloat16)
    row_max = jnp.full((heads_dev, tok_rows), -1e30, jnp.float32)
    scores = (
        jnp.einsum("qhd,khd->hqk", query_nope, keys_nope, preferred_element_type=jnp.float32)
        + jnp.einsum("qhd,kd->hqk", query_turn, pieces[1], preferred_element_type=jnp.float32)
    ) * score_scale
    new_max = jnp.maximum(row_max, jnp.max(scores, axis=-1))
    weights = jnp.exp(scores - new_max[:, :, None])
    totals = jnp.sum(weights, axis=-1)
    weighted = jnp.einsum(
        "hqk,khd->hqd",
        weights.astype(jnp.bfloat16),
        values_part,
        preferred_element_type=jnp.float32,
    )
    attended = (weighted / totals[:, :, None]).astype(jnp.bfloat16)
    attended = jnp.transpose(attended, (1, 0, 2)).reshape(tok_rows, heads_dev * value_width)
    row_share = tok_rows // lax.axis_size("tp")
    summed = lax.psum_scatter(
        jnp.dot(attended, out_weight, preferred_element_type=jnp.float32).astype(jnp.bfloat16),
        "tp",
        scatter_dimension=0,
        tiled=True,
    ).astype(jnp.float32)
    own_rows = lax.dynamic_slice_in_dim(residual, tp_index * row_share, row_share, 0).astype(
        jnp.float32
    )
    stream_wide = widened(own_rows + rms_norm(widened(summed), post_gain))
    own_inputs = rms_norm(stream_wide, pre_gain).astype(jnp.bfloat16)
    sp_size = lax.axis_size("sp")
    if up_value.shape[1] // sp_size >= 128:
        return feed_by_units(
            own_inputs, stream_wide, up_value, up_gate, conv_value, conv_gate, down_weight, ffn_gain
        )
    inputs = lax.all_gather(own_inputs, "tp", axis=0, tiled=True)
    ff_dev = up_value.shape[1]
    up_joined = jnp.concatenate([up_value, up_gate], axis=1)
    up_whole = lax.all_gather(up_joined, "sp", axis=0, tiled=True)
    up_pair = jnp.dot(inputs, up_whole, preferred_element_type=jnp.float32).astype(jnp.bfloat16)
    padded = extended(up_pair, (("sp", 0),), 1).astype(jnp.float32)
    channel_start = tp_index * ff_dev
    conv_taps = jnp.concatenate(
        [
            lax.dynamic_slice_in_dim(conv_value, channel_start, ff_dev, 1),
            lax.dynamic_slice_in_dim(conv_gate, channel_start, ff_dev, 1),
        ],
        axis=1,
    ).astype(jnp.float32)
    mixed_conv = (
        padded[:-2] * conv_taps[0] + padded[1:-1] * conv_taps[1] + padded[2:] * conv_taps[2]
    )
    hidden = (jax.nn.silu(mixed_conv[:, ff_dev:]) * mixed_conv[:, :ff_dev]).astype(jnp.bfloat16)
    down_whole = lax.all_gather(down_weight, "sp", axis=1, tiled=True)
    down_terms = jnp.dot(hidden, down_whole, preferred_element_type=jnp.float32)
    reduced = lax.psum_scatter(
        down_terms.astype(jnp.bfloat16), "tp", scatter_dimension=0, tiled=True
    ).astype(jnp.float32)
    return (stream_wide + rms_norm(widened(reduced), ffn_gain)).astype(jnp.bfloat16)


def solution(mesh):
    placed = (
        P("sp", None),
        P("sp", "tp", None),
        P("sp", "tp", None),
        P("sp", None),
        P("sp", None),
        P(),
        P(),
        P(),
        P("tp", None),
        P(),
        P(),
        P(),
        P("sp", "tp"),
        P("sp", "tp"),
        P(),
        P(),
        P("tp", "sp"),
    )
    return jax.shard_map(
        body, mesh=mesh, in_specs=placed, out_specs=P(("sp", "tp"), None), check_vma=False
    )
```

```python
import jax
import jax.numpy as jnp
from jax import lax
from jax.sharding import PartitionSpec as P

GRID = 64


epsilon = 1e-06
rope_base = 10000.0


def extended(x, sides, width):
    for axis, dim in sides:
        size, length = (lax.axis_size(axis), x.shape[dim])
        up = [(i, (i + 1) % size) for i in range(size - 1)]
        down = [(j, i) for i, j in up]
        last = lax.slice_in_dim(x, length - width, length, axis=dim)
        initial = lax.slice_in_dim(x, 0, width, axis=dim)
        before = lax.ppermute(last, axis, up)
        after = lax.ppermute(initial, axis, down)
        x = jnp.concatenate([before, x, after], axis=dim)
    return x


def rms_norm(values, gain):
    return (
        values
        * lax.rsqrt(jnp.mean(values * values, axis=-1, keepdims=True) + epsilon)
        * gain.astype(jnp.float32)
    )


def widened(values):
    return lax.optimization_barrier(values.astype(jnp.bfloat16)).astype(jnp.float32)


def rotate(values, positions):
    pair_count = values.shape[-1] // 4
    frequency = rope_base ** (-jnp.arange(pair_count, dtype=jnp.float32) / pair_count)
    grid_rows = (positions // GRID).astype(jnp.float32)
    grid_cols = (positions % GRID).astype(jnp.float32)
    angles = jnp.stack([grid_rows, grid_cols], axis=-1)[:, :, None] * frequency
    table_shape = (angles.shape[0],) + (1,) * (values.ndim - 2) + angles.shape[1:]
    cosine = jnp.cos(angles).reshape(table_shape)
    sine = jnp.sin(angles).reshape(table_shape)
    halves = values.reshape(values.shape[:-1] + (2, 2, pair_count))
    leading = halves[..., 0, :]
    trailing = halves[..., 1, :]
    turned = jnp.stack(
        [leading * cosine - trailing * sine, trailing * cosine + leading * sine], axis=-2
    )
    return turned.reshape(values.shape)


def spread_weights(up_value, up_gate, down_weight):
    sp_size = lax.axis_size("sp")
    unit = up_value.shape[1] // sp_size
    up_pair = jnp.stack(
        [up_value.reshape(-1, sp_size, unit), up_gate.reshape(-1, sp_size, unit)], axis=0
    )
    up_mine = lax.all_to_all(up_pair, "sp", split_axis=2, concat_axis=1, tiled=True)[:, :, 0]
    down_mine = lax.all_to_all(down_weight, "sp", split_axis=0, concat_axis=1, tiled=True)
    return up_mine, down_mine


def exchanged(parts, dim, axis, bit):
    place = (lax.axis_index(axis) // bit) % 2
    kept = lax.dynamic_index_in_dim(parts, place, dim, keepdims=False)
    sent = lax.dynamic_index_in_dim(parts, 1 - place, dim, keepdims=False)
    pairs = [(i, i ^ bit) for i in range(lax.axis_size(axis))]
    came = lax.ppermute(sent.astype(jnp.bfloat16), axis, pairs)
    return (kept.astype(jnp.float32) + came.astype(jnp.float32)).astype(jnp.bfloat16)


def scattered_sum(hidden, down):
    bits = lax.axis_size("sp").bit_length() - 1
    share = hidden.shape[0] // (2 * lax.axis_size("sp"))
    place = lax.axis_index("tp")
    rows = hidden.reshape(-1, 2, share, hidden.shape[1])

    def product(side, cols):
        picked = lax.dynamic_index_in_dim(rows, side, 1, keepdims=False)
        return jnp.dot(
            picked.reshape(-1, hidden.shape[1]), cols, preferred_element_type=jnp.float32
        )

    half = down.shape[1] // 2
    halves = [down[:, :half], down[:, half:]]
    sent = [product(1 - place, cols).astype(jnp.bfloat16) for cols in halves]
    came = [lax.ppermute(part, "tp", [(0, 1), (1, 0)]) for part in sent]
    parts = [
        (product(place, cols) + part.astype(jnp.float32))
        .astype(jnp.bfloat16)
        .reshape((2,) * bits + (share, half))
        for cols, part in zip(halves, came)
    ]
    orders = [list(range(bits)), [1, 0] + list(range(2, bits))]
    left = [list(range(bits - 1, -1, -1)) for _ in parts]
    for step in range(bits):
        for i, order in enumerate(orders):
            bit = order[step]
            parts[i] = exchanged(parts[i], left[i].index(bit), "sp", 1 << bit)
            left[i].remove(bit)
    return jnp.concatenate(parts, axis=1)


def feed_by_units(
    own_inputs, stream_wide, up_mine, down_mine, conv_value, conv_gate, ff_dev, ffn_gain
):
    sp_size = lax.axis_size("sp")
    unit = ff_dev // sp_size
    first_unit = lax.axis_index("tp") * ff_dev + lax.axis_index("sp") * unit
    inputs = lax.all_gather(own_inputs, ("sp", "tp"), axis=0, tiled=True)

    def conved(weight, taps):
        rows = jnp.dot(inputs, weight, preferred_element_type=jnp.float32).astype(jnp.bfloat16)
        padded = jnp.pad(rows, ((1, 1), (0, 0))).astype(jnp.float32)
        taps = lax.dynamic_slice_in_dim(taps, first_unit, unit, 1).astype(jnp.float32)
        return padded[:-2] * taps[0] + padded[1:-1] * taps[1] + padded[2:] * taps[2]

    hidden = jax.nn.silu(conved(up_mine[1], conv_gate)) * conved(up_mine[0], conv_value)
    reduced = scattered_sum(hidden.astype(jnp.bfloat16), down_mine)
    reduced = widened(reduced.astype(jnp.float32))
    return (stream_wide + rms_norm(reduced, ffn_gain)).astype(jnp.bfloat16)


def body(
    residual,
    query_nope,
    query_rope,
    latent,
    rope_key,
    kv_gain,
    key_up,
    value_up,
    out_weight,
    post_gain,
    pre_gain,
    ffn_gain,
    up_value,
    up_gate,
    conv_value,
    conv_gate,
    down_weight,
):
    tok_rows = residual.shape[0]
    heads_dev = query_nope.shape[1]
    value_width = value_up.shape[2]
    tp_index = lax.axis_index("tp")
    positions = lax.axis_index("sp") * tok_rows + jnp.arange(tok_rows, dtype=jnp.int32)
    score_scale = (query_nope.shape[2] + query_rope.shape[2]) ** (-0.5)
    normed = rms_norm(latent.astype(jnp.float32), kv_gain).astype(jnp.bfloat16)
    key_turn = rotate(rope_key.astype(jnp.float32), positions).astype(jnp.bfloat16)
    query_turn = rotate(query_rope.astype(jnp.float32), positions).astype(jnp.bfloat16)
    key_local = lax.dynamic_slice_in_dim(key_up, tp_index * heads_dev, heads_dev, 1)
    value_local = lax.dynamic_slice_in_dim(value_up, tp_index * heads_dev, heads_dev, 1)
    latent_width = normed.shape[1]
    joined = lax.all_gather(
        jnp.concatenate([normed, key_turn], axis=1), "sp", axis=0, tiled=True
    )
    pieces = (joined[:, :latent_width], joined[:, latent_width:])
    sp_size = lax.axis_size("sp")
    power_of_two = sp_size & (sp_size - 1) == 0
    by_units = (
        up_value.shape[1] // sp_size >= 128 and power_of_two and lax.axis_size("tp") == 2
    )
    if by_units:
        spread = spread_weights(up_value, up_gate, down_weight)
    keys_nope = jnp.einsum(
        "nc,chd->nhd", pieces[0], key_local, preferred_element_type=jnp.float32
    ).astype(jnp.bfloat16)
    values_part = jnp.einsum(
        "nc,chd->nhd", pieces[0], value_local, preferred_element_type=jnp.float32
    ).astype(jnp.bfloat16)
    row_max = jnp.full((heads_dev, tok_rows), -1e30, jnp.float32)
    scores = (
        jnp.einsum("qhd,khd->hqk", query_nope, keys_nope, preferred_element_type=jnp.float32)
        + jnp.einsum("qhd,kd->hqk", query_turn, pieces[1], preferred_element_type=jnp.float32)
    ) * score_scale
    new_max = jnp.maximum(row_max, jnp.max(scores, axis=-1))
    weights = jnp.exp(scores - new_max[:, :, None])
    totals = jnp.sum(weights, axis=-1)
    weighted = jnp.einsum(
        "hqk,khd->hqd",
        weights.astype(jnp.bfloat16),
        values_part,
        preferred_element_type=jnp.float32,
    )
    attended = (weighted / totals[:, :, None]).astype(jnp.bfloat16)
    attended = jnp.transpose(attended, (1, 0, 2)).reshape(tok_rows, heads_dev * value_width)
    if by_units:
        attended, spread = lax.optimization_barrier((attended, spread))
    row_share = tok_rows // lax.axis_size("tp")
    summed = lax.psum_scatter(
        jnp.dot(attended, out_weight, preferred_element_type=jnp.float32).astype(jnp.bfloat16),
        "tp",
        scatter_dimension=0,
        tiled=True,
    ).astype(jnp.float32)
    own_rows = lax.dynamic_slice_in_dim(residual, tp_index * row_share, row_share, 0).astype(
        jnp.float32
    )
    stream_wide = widened(own_rows + rms_norm(widened(summed), post_gain))
    own_inputs = rms_norm(stream_wide, pre_gain).astype(jnp.bfloat16)
    if by_units:
        return feed_by_units(
            own_inputs, stream_wide, *spread, conv_value, conv_gate, up_value.shape[1], ffn_gain
        )
    inputs = lax.all_gather(own_inputs, "tp", axis=0, tiled=True)
    ff_dev = up_value.shape[1]
    up_joined = jnp.concatenate([up_value, up_gate], axis=1)
    up_whole = lax.all_gather(up_joined, "sp", axis=0, tiled=True)
    up_pair = jnp.dot(inputs, up_whole, preferred_element_type=jnp.float32).astype(jnp.bfloat16)
    padded = extended(up_pair, (("sp", 0),), 1).astype(jnp.float32)
    channel_start = tp_index * ff_dev
    conv_taps = jnp.concatenate(
        [
            lax.dynamic_slice_in_dim(conv_value, channel_start, ff_dev, 1),
            lax.dynamic_slice_in_dim(conv_gate, channel_start, ff_dev, 1),
        ],
        axis=1,
    ).astype(jnp.float32)
    mixed_conv = (
        padded[:-2] * conv_taps[0] + padded[1:-1] * conv_taps[1] + padded[2:] * conv_taps[2]
    )
    hidden = (jax.nn.silu(mixed_conv[:, ff_dev:]) * mixed_conv[:, :ff_dev]).astype(jnp.bfloat16)
    down_whole = lax.all_gather(down_weight, "sp", axis=1, tiled=True)
    down_terms = jnp.dot(hidden, down_whole, preferred_element_type=jnp.float32)
    reduced = lax.psum_scatter(
        down_terms.astype(jnp.bfloat16), "tp", scatter_dimension=0, tiled=True
    ).astype(jnp.float32)
    return (stream_wide + rms_norm(widened(reduced), ffn_gain)).astype(jnp.bfloat16)


def solution(mesh):
    placed = (
        P("sp", None),
        P("sp", "tp", None),
        P("sp", "tp", None),
        P("sp", None),
        P("sp", None),
        P(),
        P(),
        P(),
        P("tp", None),
        P(),
        P(),
        P(),
        P("sp", "tp"),
        P("sp", "tp"),
        P(),
        P(),
        P("tp", "sp"),
    )
    return jax.shard_map(
        body, mesh=mesh, in_specs=placed, out_specs=P(("sp", "tp"), None), check_vma=False
    )
```

```python
import jax
import jax.numpy as jnp
from jax import lax
from jax.sharding import PartitionSpec as P

GRID = 64


epsilon = 1e-06
rope_base = 10000.0


def extended(x, sides, width):
    for axis, dim in sides:
        size, length = (lax.axis_size(axis), x.shape[dim])
        up = [(i, (i + 1) % size) for i in range(size - 1)]
        down = [(j, i) for i, j in up]
        last = lax.slice_in_dim(x, length - width, length, axis=dim)
        initial = lax.slice_in_dim(x, 0, width, axis=dim)
        before = lax.ppermute(last, axis, up)
        after = lax.ppermute(initial, axis, down)
        x = jnp.concatenate([before, x, after], axis=dim)
    return x


def rms_norm(values, gain):
    return (
        values
        * lax.rsqrt(jnp.mean(values * values, axis=-1, keepdims=True) + epsilon)
        * gain.astype(jnp.float32)
    )


def widened(values):
    return lax.optimization_barrier(values.astype(jnp.bfloat16)).astype(jnp.float32)


def rotate(values, positions):
    pair_count = values.shape[-1] // 4
    frequency = rope_base ** (-jnp.arange(pair_count, dtype=jnp.float32) / pair_count)
    grid_rows = (positions // GRID).astype(jnp.float32)
    grid_cols = (positions % GRID).astype(jnp.float32)
    angles = jnp.stack([grid_rows, grid_cols], axis=-1)[:, :, None] * frequency
    table_shape = (angles.shape[0],) + (1,) * (values.ndim - 2) + angles.shape[1:]
    cosine = jnp.cos(angles).reshape(table_shape)
    sine = jnp.sin(angles).reshape(table_shape)
    halves = values.reshape(values.shape[:-1] + (2, 2, pair_count))
    leading = halves[..., 0, :]
    trailing = halves[..., 1, :]
    turned = jnp.stack(
        [leading * cosine - trailing * sine, trailing * cosine + leading * sine], axis=-2
    )
    return turned.reshape(values.shape)


def side_groups():
    size = lax.axis_size("sp")
    return [list(range(side, size, 2)) for side in range(2)]


def swapped(x):
    return lax.ppermute(x, "sp", [(i, i ^ 1) for i in range(lax.axis_size("sp"))])


def paired(mine, dim):
    other = swapped(mine)
    is_first = lax.axis_index("sp") % 2 == 0
    return jnp.stack(
        [jnp.where(is_first, mine, other), jnp.where(is_first, other, mine)], axis=dim
    )


def gathered_by_doubling(x):
    size = lax.axis_size("sp")
    bits = size.bit_length() - 1
    half = x.shape[0] // 2
    orders = [list(range(bits - 1, -1, -1)), list(range(bits - 1, 1, -1)) + [0, 1]]
    parts = [x[:half], x[half:]]
    for step in range(bits):
        for i, order in enumerate(orders):
            bit = order[step]
            mine = parts[i]
            other = lax.ppermute(mine, "sp", [(j, j ^ (1 << bit)) for j in range(size)])
            is_first = (lax.axis_index("sp") >> bit) % 2 == 0
            parts[i] = jnp.stack(
                [jnp.where(is_first, mine, other), jnp.where(is_first, other, mine)],
                axis=sum(done > bit for done in order[:step]),
            )
    parts = [part.reshape(size, half, x.shape[1]) for part in parts]
    return jnp.concatenate(parts, axis=1).reshape(-1, x.shape[1])


def spread_weights(up_value, up_gate, down_weight):
    places = lax.axis_size("sp") // 2
    depth, ff_dev = up_value.shape
    unit = ff_dev // places

    def sent(x):
        return lax.all_to_all(
            x, "sp", split_axis=0, concat_axis=0, axis_index_groups=side_groups(), tiled=True
        )

    up_pair = jnp.concatenate(
        [up_value.reshape(depth, places, unit), up_gate.reshape(depth, places, unit)], axis=2
    )
    up_mine = paired(sent(jnp.transpose(up_pair, (1, 0, 2))), 1)
    down_mine = paired(sent(down_weight.reshape(places, unit, -1)), 1)
    down_mine = jnp.transpose(down_mine, (2, 0, 1, 3))
    return up_mine.reshape(-1, 2 * unit), down_mine.reshape(unit, -1)


def exchanged(parts, dim, axis, bit):
    place = (lax.axis_index(axis) // bit) % 2
    kept = lax.dynamic_index_in_dim(parts, place, dim, keepdims=False)
    sent = lax.dynamic_index_in_dim(parts, 1 - place, dim, keepdims=False)
    pairs = [(i, i ^ bit) for i in range(lax.axis_size(axis))]
    came = lax.ppermute(sent.astype(jnp.bfloat16), axis, pairs)
    return (kept.astype(jnp.float32) + came.astype(jnp.float32)).astype(jnp.bfloat16)


def scattered_sum(hidden, down):
    bits = lax.axis_size("sp").bit_length() - 2
    share = hidden.shape[0] // lax.axis_size("sp")
    place = lax.axis_index("tp")
    rows = hidden.reshape(-1, 2, share, hidden.shape[1])

    def product(side, cols):
        picked = lax.dynamic_index_in_dim(rows, side, 1, keepdims=False)
        return jnp.dot(
            picked.reshape(-1, hidden.shape[1]), cols, preferred_element_type=jnp.float32
        )

    half = down.shape[1] // 2
    halves = [down[:, :half], down[:, half:]]
    sent = [product(1 - place, cols).astype(jnp.bfloat16) for cols in halves]
    came = [lax.ppermute(part, "tp", [(0, 1), (1, 0)]) for part in sent]
    parts = [
        (product(place, cols) + part.astype(jnp.float32))
        .astype(jnp.bfloat16)
        .reshape((2,) * bits + (share, half))
        for cols, part in zip(halves, came)
    ]
    orders = [list(range(1, bits + 1)), [2, 1] + list(range(3, bits + 1))]
    left = [list(range(bits, 0, -1)) for _ in parts]
    for step in range(bits):
        for i, order in enumerate(orders):
            bit = order[step]
            parts[i] = exchanged(parts[i], left[i].index(bit), "sp", 1 << bit)
            left[i].remove(bit)
    return jnp.concatenate(parts, axis=1)


def feed_by_units(
    own_inputs, stream_wide, up_mine, down_mine, conv_value, conv_gate, ff_dev, ffn_gain
):
    places = lax.axis_size("sp") // 2
    share = own_inputs.shape[0]
    unit = ff_dev // places
    side = lax.axis_index("sp") % 2
    is_first = side == 0
    tp_index = lax.axis_index("tp")
    first_unit = tp_index * ff_dev + lax.axis_index("sp") // 2 * unit
    edge = lax.dynamic_slice_in_dim(own_inputs, tp_index * (share - 1), 1, 0)
    edge = swapped(jnp.pad(edge, ((0, 7), (0, 0))))
    groups = [[2 * i + t for i in group for t in range(2)] for group in side_groups()]
    blocks = lax.all_gather(
        jnp.concatenate([own_inputs, edge], axis=0),
        ("sp", "tp"),
        axis=0,
        tiled=True,
        axis_index_groups=groups,
    )
    rows = jnp.dot(blocks, up_mine, preferred_element_type=jnp.float32).astype(jnp.bfloat16)
    rows = rows.reshape(places, 2, share + 8, 2 * unit)
    blank = jnp.zeros((1, 2 * unit), rows.dtype)
    first_rows, last_rows = rows[:, 0, share], rows[:, 1, share]
    before = jnp.where(is_first, jnp.concatenate([blank, last_rows[:-1]], axis=0), last_rows)
    after = jnp.where(is_first, first_rows, jnp.concatenate([first_rows[1:], blank], axis=0))
    main = rows[:, :, :share].reshape(places, 2 * share, 2 * unit)
    padded = jnp.concatenate([before[:, None], main, after[:, None]], axis=1).astype(jnp.float32)
    taps = jnp.concatenate(
        [
            lax.dynamic_slice_in_dim(conv_value, first_unit, unit, 1),
            lax.dynamic_slice_in_dim(conv_gate, first_unit, unit, 1),
        ],
        axis=1,
    ).astype(jnp.float32)
    mixed = padded[:, :-2] * taps[0] + padded[:, 1:-1] * taps[1] + padded[:, 2:] * taps[2]
    hidden = jax.nn.silu(mixed[..., unit:]) * mixed[..., :unit]
    hidden = hidden.reshape(-1, unit)
    reduced = scattered_sum(hidden.astype(jnp.bfloat16), down_mine)
    reduced = widened(reduced.astype(jnp.float32))
    return (stream_wide + rms_norm(reduced, ffn_gain)).astype(jnp.bfloat16)


def body(
    residual,
    query_nope,
    query_rope,
    latent,
    rope_key,
    kv_gain,
    key_up,
    value_up,
    out_weight,
    post_gain,
    pre_gain,
    ffn_gain,
    up_value,
    up_gate,
    conv_value,
    conv_gate,
    down_weight,
):
    tok_rows = residual.shape[0]
    heads_dev = query_nope.shape[1]
    value_width = value_up.shape[2]
    tp_index = lax.axis_index("tp")
    positions = lax.axis_index("sp") * tok_rows + jnp.arange(tok_rows, dtype=jnp.int32)
    score_scale = (query_nope.shape[2] + query_rope.shape[2]) ** (-0.5)
    normed = rms_norm(latent.astype(jnp.float32), kv_gain).astype(jnp.bfloat16)
    key_turn = rotate(rope_key.astype(jnp.float32), positions).astype(jnp.bfloat16)
    query_turn = rotate(query_rope.astype(jnp.float32), positions).astype(jnp.bfloat16)
    key_local = lax.dynamic_slice_in_dim(key_up, tp_index * heads_dev, heads_dev, 1)
    value_local = lax.dynamic_slice_in_dim(value_up, tp_index * heads_dev, heads_dev, 1)
    latent_width = normed.shape[1]
    joined = jnp.concatenate([normed, key_turn], axis=1)
    sp_size = lax.axis_size("sp")
    power_of_two = sp_size & (sp_size - 1) == 0
    by_units = (
        sp_size >= 8 and up_value.shape[1] // sp_size >= 128 and power_of_two and lax.axis_size("tp") == 2
    )
    if by_units:
        joined = gathered_by_doubling(joined)
        spread = spread_weights(up_value, up_gate, down_weight)
    else:
        joined = lax.all_gather(joined, "sp", axis=0, tiled=True)
    pieces = (joined[:, :latent_width], joined[:, latent_width:])
    keys_nope = jnp.einsum(
        "nc,chd->nhd", pieces[0], key_local, preferred_element_type=jnp.float32
    ).astype(jnp.bfloat16)
    values_part = jnp.einsum(
        "nc,chd->nhd", pieces[0], value_local, preferred_element_type=jnp.float32
    ).astype(jnp.bfloat16)
    row_max = jnp.full((heads_dev, tok_rows), -1e30, jnp.float32)
    scores = (
        jnp.einsum("qhd,khd->hqk", query_nope, keys_nope, preferred_element_type=jnp.float32)
        + jnp.einsum("qhd,kd->hqk", query_turn, pieces[1], preferred_element_type=jnp.float32)
    ) * score_scale
    new_max = jnp.maximum(row_max, jnp.max(scores, axis=-1))
    weights = jnp.exp(scores - new_max[:, :, None])
    totals = jnp.sum(weights, axis=-1)
    weighted = jnp.einsum(
        "hqk,khd->hqd",
        weights.astype(jnp.bfloat16),
        values_part,
        preferred_element_type=jnp.float32,
    )
    attended = (weighted / totals[:, :, None]).astype(jnp.bfloat16)
    attended = jnp.transpose(attended, (1, 0, 2)).reshape(tok_rows, heads_dev * value_width)
    if by_units:
        attended, spread = lax.optimization_barrier((attended, spread))
    row_share = tok_rows // lax.axis_size("tp")
    summed = lax.psum_scatter(
        jnp.dot(attended, out_weight, preferred_element_type=jnp.float32).astype(jnp.bfloat16),
        "tp",
        scatter_dimension=0,
        tiled=True,
    ).astype(jnp.float32)
    own_rows = lax.dynamic_slice_in_dim(residual, tp_index * row_share, row_share, 0).astype(
        jnp.float32
    )
    stream_wide = widened(own_rows + rms_norm(widened(summed), post_gain))
    own_inputs = rms_norm(stream_wide, pre_gain).astype(jnp.bfloat16)
    if by_units:
        return feed_by_units(
            own_inputs, stream_wide, *spread, conv_value, conv_gate, up_value.shape[1], ffn_gain
        )
    inputs = lax.all_gather(own_inputs, "tp", axis=0, tiled=True)
    ff_dev = up_value.shape[1]
    up_joined = jnp.concatenate([up_value, up_gate], axis=1)
    up_whole = lax.all_gather(up_joined, "sp", axis=0, tiled=True)
    up_pair = jnp.dot(inputs, up_whole, preferred_element_type=jnp.float32).astype(jnp.bfloat16)
    padded = extended(up_pair, (("sp", 0),), 1).astype(jnp.float32)
    channel_start = tp_index * ff_dev
    conv_taps = jnp.concatenate(
        [
            lax.dynamic_slice_in_dim(conv_value, channel_start, ff_dev, 1),
            lax.dynamic_slice_in_dim(conv_gate, channel_start, ff_dev, 1),
        ],
        axis=1,
    ).astype(jnp.float32)
    mixed_conv = (
        padded[:-2] * conv_taps[0] + padded[1:-1] * conv_taps[1] + padded[2:] * conv_taps[2]
    )
    hidden = (jax.nn.silu(mixed_conv[:, ff_dev:]) * mixed_conv[:, :ff_dev]).astype(jnp.bfloat16)
    down_whole = lax.all_gather(down_weight, "sp", axis=1, tiled=True)
    down_terms = jnp.dot(hidden, down_whole, preferred_element_type=jnp.float32)
    reduced = lax.psum_scatter(
        down_terms.astype(jnp.bfloat16), "tp", scatter_dimension=0, tiled=True
    ).astype(jnp.float32)
    return (stream_wide + rms_norm(widened(reduced), ffn_gain)).astype(jnp.bfloat16)


def solution(mesh):
    placed = (
        P("sp", None),
        P("sp", "tp", None),
        P("sp", "tp", None),
        P("sp", None),
        P("sp", None),
        P(),
        P(),
        P(),
        P("tp", None),
        P(),
        P(),
        P(),
        P("sp", "tp"),
        P("sp", "tp"),
        P(),
        P(),
        P("tp", "sp"),
    )
    return jax.shard_map(
        body, mesh=mesh, in_specs=placed, out_specs=P(("sp", "tp"), None), check_vma=False
    )
```
